512 devices in a mesh: fs: 16 (over y, x), tp: 32 (over z, core).
Axes of the slice: x: 4, y: 4, z: 16, core: 2. Of those that a mesh axis runs over, the one named last changes fastest.
Arguments:
- saved_input: bfloat16 [16384, 4096], P('fs', 'tp'), may hold values from -6 to 6
- query_cot: bfloat16 [16384, 4096], P('fs', 'tp'), may hold values from -6 to 6
- key_cot: bfloat16 [16384, 4096], P('fs', 'tp'), may hold values from -6 to 6
- query_master: float32 [4096, 4096], P('fs', 'tp'), may hold values from -0.09375 to 0.09375
- key_master: float32 [4096, 4096], P('fs', 'tp'), may hold values from -0.09375 to 0.09375
- query_basis: bfloat16 [4096, 256], P('fs'), may hold values from -3 to 3
- key_basis: bfloat16 [4096, 256], P('fs'), may hold values from -3 to 3
- query_first: float32 [256, 4096], P('fs', 'tp'), may hold values from -240 to 240
- query_second: float32 [256, 4096], P('fs', 'tp'), may hold values from 1000 to 20000
- key_first: float32 [256, 4096], P('fs', 'tp'), may hold values from -240 to 240
- key_second: float32 [256, 4096], P('fs', 'tp'), may hold values from 1000 to 20000
Outputs:
- query_step: float32 [4096, 4096], P('fs', 'tp')
- query_weight: float32 [4096, 4096], P('fs', 'tp')
- query_copy: bfloat16 [4096, 4096], P(None, 'tp')
- query_first_new: float32 [256, 4096], P('fs', 'tp')
- query_second_new: float32 [256, 4096], P('fs', 'tp')
- key_step: float32 [4096, 4096], P('fs', 'tp')
- key_weight: float32 [4096, 4096], P('fs', 'tp')
- key_copy: bfloat16 [4096, 4096], P(None, 'tp')
- key_first_new: float32 [256, 4096], P('fs', 'tp')
- key_second_new: float32 [256, 4096], P('fs', 'tp')
The draws below stay inside these ranges and needn't reach their ends.
All inputs are finite; a program needn't handle non-finite values.
Results may differ from the reference program's by a relative error of at most 0.0065.
Values may be sent and summed in bfloat16 or wider, within the bound.
No kernel may reach another device: no remote copies, remote signals or barrier semaphores. Data moves between devices by JAX's collectives and lax.ppermute only.
A program may use at most 64 MiB of HBM per device.

```python
import math
import jax
import jax.numpy as jnp
from jax import lax

D = 4096
HEADS = 32
HD = 128
RANK = 256
TOKENS = 16384


def basis_draw(key, salt):
    base = jax.random.fold_in(key, salt)
    entry_key, factor_key = jax.random.split(base)
    group = max(D // 64, 1)
    groups = D // group
    entries = jnp.clip(jax.random.normal(entry_key, (D, RANK), jnp.float32), -4.0, 4.0)
    factors = jnp.exp(jax.random.uniform(factor_key, (groups,), jnp.float32, -1.5, 1.5))
    row_scale = jnp.repeat(factors, group)
    values = entries * row_scale[:, None] * D ** (-0.5)
    return values.astype(jnp.bfloat16)


def draw_query_basis(key, part):
    return basis_draw(key, 101)


def draw_key_basis(key, part):
    return basis_draw(key, 202)


def block_scale(key, dims, pieces, low, largest):
    loudness, own = 1.0, jax.random.fold_in(key, 6)
    for position, blocks in pieces:
        steps = jnp.exp(jax.random.uniform(jax.random.fold_in(own, position), (blocks,), jnp.float32, low / len(pieces), largest / len(pieces)))
        loudness = loudness * jnp.repeat(steps, dims[position] // blocks).reshape([-1 if axis == position else 1 for axis in range(len(dims))])
    return loudness


def bell_draw(stream_key, shape, scale, most, cuts=(), kind=jnp.bfloat16):
    values = jax.random.normal(stream_key, shape, jnp.float32) * scale
    if len(cuts) > 0:
        values = block_scale(stream_key, shape, cuts, -0.22, 0.18) * values
    return jnp.clip(values, min=-most, max=most).astype(kind)


def setup_inputs(seed: int = 0) -> dict:
    seeds = jax.random.split(jax.random.key(seed), 12)
    saved_input = bell_draw(seeds[0], (TOKENS, D), 1.0, 6.0, ((0, 16), (1, 32)))
    query_cot = bell_draw(seeds[1], (TOKENS, HEADS * HD), 1.0, 6.0, ((0, 16), (1, 32)))
    key_cot = bell_draw(seeds[2], (TOKENS, HEADS * HD), 1.0, 6.0, ((0, 16), (1, 32)))
    query_master = bell_draw(seeds[3], (D, HEADS * HD), D ** -0.5, 0.09375, ((0, 16), (1, 32)), jnp.float32)
    key_master = bell_draw(seeds[4], (D, HEADS * HD), D ** -0.5, 0.09375, ((0, 16), (1, 32)), jnp.float32)
    query_basis = draw_query_basis(jax.random.fold_in(seeds[11], 71), 0)
    key_basis = draw_key_basis(jax.random.fold_in(seeds[11], 71), 0)
    query_first = bell_draw(seeds[7], (RANK, HEADS * HD), 40.0, 240.0, ((0, 16), (1, 32)), jnp.float32)
    query_second = jnp.clip(jnp.exp(math.log(20000.0) - 2.9957323 * jax.random.uniform(seeds[8], (RANK, HEADS * HD), jnp.float32) ** block_scale(seeds[8], (RANK, HEADS * HD), ((0, 16), (1, 32)), -0.2, 0.2)), 1000.0, 20000.0)
    key_first = bell_draw(seeds[9], (RANK, HEADS * HD), 40.0, 240.0, ((0, 16), (1, 32)), jnp.float32)
    key_second = jnp.clip(jnp.exp(math.log(20000.0) - 2.9957323 * jax.random.uniform(seeds[10], (RANK, HEADS * HD), jnp.float32) ** block_scale(seeds[10], (RANK, HEADS * HD), ((0, 16), (1, 32)), -0.2, 0.2)), 1000.0, 20000.0)
    return {"saved_input": saved_input, "query_cot": query_cot, "key_cot": key_cot, "query_master": query_master, "key_master": key_master, "query_basis": query_basis, "key_basis": key_basis, "query_first": query_first, "query_second": query_second, "key_first": key_first, "key_second": key_second}


moment_decay = 0.8
square_decay = 0.9
square_floor = 1.0
norm_floor = 0.01
step_rate = 0.01

def update_one(saved_input, cotangent, master, basis, first, second):
    grad = jnp.dot(saved_input.T, cotangent, preferred_element_type=jnp.float32)
    low = jnp.dot(basis.astype(jnp.float32).T, grad, precision=lax.Precision.HIGHEST)
    first_new = moment_decay * first + (1.0 - moment_decay) * low
    second_new = square_decay * second + (1.0 - square_decay) * low * low
    ratio = (first_new / jnp.sqrt(second_new + square_floor)).astype(jnp.bfloat16)
    update = jnp.dot(basis, ratio, preferred_element_type=jnp.float32)
    by_head = update.reshape(D, HEADS, HD)
    head_mean = lax.optimization_barrier(jnp.mean(by_head * by_head, axis=(0, 2)))
    head_scale = 1.0 / jnp.sqrt(head_mean + norm_floor)
    step = (by_head * head_scale[None, :, None]).reshape(D, HEADS * HD)
    weight = master - step_rate * step
    return (step, weight, weight.astype(jnp.bfloat16), first_new, second_new)

def reference(saved_input, query_cot, key_cot, query_master, key_master, query_basis, key_basis, query_first, query_second, key_first, key_second):
    query_out = update_one(saved_input, query_cot, query_master, query_basis, query_first, query_second)
    key_out = update_one(saved_input, key_cot, key_master, key_basis, key_first, key_second)
    return (query_out[0], query_out[1], query_out[2], query_out[3], query_out[4], key_out[0], key_out[1], key_out[2], key_out[3], key_out[4])
```

```python
import jax
import jax.numpy as jnp
from jax import lax
from jax.sharding import Mesh
from jax.sharding import PartitionSpec as P

D = 4096
HD = 128
FS = ("y", "x")


moment_decay = 0.8
square_decay = 0.9
square_floor = 1.0
norm_floor = 0.01
step_rate = 0.01


def sent_to_all(x, axis):
    count = lax.axis_size(axis)
    return lax.all_to_all(jnp.broadcast_to(x[None], (count, *x.shape)), axis, 0, 0, tiled=True)


def body(
    saved_input,
    query_cot,
    key_cot,
    query_master,
    key_master,
    query_basis,
    key_basis,
    query_first,
    query_second,
    key_first,
    key_second,
):
    rows = lax.axis_size(FS)
    depth = lax.axis_size("z")
    tokens, width = query_cot.shape
    low_count = query_first.shape[0]
    share = tokens // depth
    first_core = lax.axis_index("c") == 0

    own_basis = jnp.where(first_core, query_basis, key_basis)
    basis = sent_to_all(own_basis, FS).reshape(D, -1)
    pieces = lax.all_to_all(saved_input.reshape(depth, share, width), "z", 0, 0, tiled=True)
    pieces = lax.all_gather(pieces, "c", axis=0, tiled=False)
    inputs = pieces.transpose(2, 1, 0, 3).reshape(share, D)
    low = jnp.dot(inputs, basis, preferred_element_type=jnp.float32).astype(jnp.bfloat16)
    low = lax.all_gather(low, "z", axis=0, tiled=True)
    cots = lax.all_to_all(jnp.stack([query_cot, key_cot]), "c", 0, 0, tiled=True)
    partial = [
        lax.dot_general(low, cots[h], (((0,), (0,)), ((), ())), preferred_element_type=jnp.float32)
        .reshape(rows, low_count, width)
        for h in range(2)
    ]
    partial = jnp.stack(partial, axis=1).reshape(2 * rows, low_count, width)
    partial = lax.all_to_all(partial, (*FS, "c"), 0, 0, tiled=True)
    projected = jnp.sum(partial.reshape(rows, 2, low_count, width), axis=0)

    firsts = jnp.stack([query_first, key_first])
    seconds = jnp.stack([query_second, key_second])
    first_new = moment_decay * firsts + (1.0 - moment_decay) * projected
    second_new = square_decay * seconds + (1.0 - square_decay) * projected * projected
    ratio = (first_new / jnp.sqrt(second_new + square_floor)).astype(jnp.bfloat16)
    ratio = sent_to_all(ratio, FS).transpose(1, 0, 2, 3).reshape(2, rows * low_count, width)

    bases = sent_to_all(basis, "c")
    masters = sent_to_all(jnp.stack([query_master, key_master]).astype(jnp.bfloat16), FS)
    outs = []
    for k, (own, master) in enumerate(((query_basis, query_master), (key_basis, key_master))):
        update = jnp.dot(bases[k], ratio[k], preferred_element_type=jnp.float32)
        scale = 1.0 / jnp.sqrt(jnp.sum(update * update) / (D * HD) + norm_floor)
        whole = masters[:, k].reshape(D, width).astype(jnp.float32)
        copy = (whole - step_rate * (update * scale)).astype(jnp.bfloat16)
        step = jnp.dot(own, ratio[k], preferred_element_type=jnp.float32) * scale
        weight = master - step_rate * step
        outs += [step, weight, copy, first_new[k], second_new[k]]
    return tuple(outs)


def solution(mesh):
    torus = Mesh(mesh.devices.reshape(4, 4, 16, 2), ("y", "x", "z", "c"))
    tp = ("z", "c")
    split = P(FS, tp)
    rows = P(FS, None)
    copied = P(None, tp)
    in_specs = (split,) * 5 + (rows,) * 2 + (split,) * 4
    out_specs = (split, split, copied, split, split) * 2
    return jax.shard_map(body, mesh=torus, in_specs=in_specs, out_specs=out_specs, check_vma=False)
```

```python
import jax
import jax.numpy as jnp
from jax import lax
from jax.experimental import pallas as pl
from jax.experimental.pallas import tpu as pltpu
from jax.sharding import Mesh
from jax.sharding import PartitionSpec as P


D = 4096
HD = 128
FS = ("y", "x")
BF = jnp.bfloat16
F32 = jnp.float32

moment_decay = 0.8
square_decay = 0.9
square_floor = 1.0
norm_floor = 0.01
step_rate = 0.01

VMEM = pltpu.CompilerParams(vmem_limit_bytes=48 * 1024 * 1024)


def sent_to_all(x, axis):
    count = lax.axis_size(axis)
    return lax.all_to_all(jnp.broadcast_to(x[None], (count, *x.shape)), axis, 0, 0, tiled=True)


def swapped(x, axis):
    count = lax.axis_size(axis)
    return lax.ppermute(x, axis, [(i, i ^ 1) for i in range(count)])


def product_kernel(core_ref, own_ref, other_ref, basis_ref, out_ref):
    core = core_ref[0]
    total = jnp.zeros(out_ref.shape, F32)
    for z in range(own_ref.shape[0]):
        total += jnp.dot(own_ref[z], basis_ref[z, core], preferred_element_type=F32)
        total += jnp.dot(other_ref[z], basis_ref[z, 1 - core], preferred_element_type=F32)
    out_ref[...] = total.astype(out_ref.dtype)


def product(core, own, other, basis):
    depth, share, width = own.shape
    basis = basis.reshape(depth, 2, width, basis.shape[-1])
    return pl.pallas_call(
        product_kernel,
        out_shape=jax.ShapeDtypeStruct((share, basis.shape[-1]), BF),
        in_specs=[pl.BlockSpec(memory_space=pltpu.SMEM)] + [pl.BlockSpec(memory_space=pltpu.VMEM)] * 3,
        compiler_params=VMEM,
        name="product",
    )(core, own, other, basis)


def partial_kernel(core_ref, low_ref, own_ref, other_ref, out_ref):
    core = core_ref[0]
    chunks, halves, share, ranks = low_ref.shape
    rows, _, count, width = out_ref.shape
    per = rows // halves
    for half in range(halves):
        mine = jnp.zeros((ranks, width), F32)
        theirs = jnp.zeros((ranks, width), F32)
        for chunk in range(chunks):
            part = low_ref[chunk, half]
            span = pl.ds(chunk * share, share)
            contract = (((0,), (0,)), ((), ()))
            mine += lax.dot_general(part, own_ref[span, :], contract, preferred_element_type=F32)
            theirs += lax.dot_general(part, other_ref[span, :], contract, preferred_element_type=F32)
        span = pl.ds(half * per, per)
        out_ref[span, core] = mine.reshape(per, count, width).astype(out_ref.dtype)
        out_ref[span, 1 - core] = theirs.reshape(per, count, width).astype(out_ref.dtype)


def partials(core, low, own, other, rows, count):
    return pl.pallas_call(
        partial_kernel,
        out_shape=jax.ShapeDtypeStruct((rows, 2, count, own.shape[-1]), BF),
        in_specs=[pl.BlockSpec(memory_space=pltpu.SMEM)] + [pl.BlockSpec(memory_space=pltpu.VMEM)] * 3,
        compiler_params=VMEM,
        name="partials",
    )(core, low, own, other)


BLOCK = 512


def finish_kernel(
    place_ref,
    ratio_ref,
    own_a_ref,
    own_b_ref,
    other_a_ref,
    other_b_ref,
    masters_ref,
    query_master_ref,
    key_master_ref,
    query_step_ref,
    query_weight_ref,
    query_copy_ref,
    key_step_ref,
    key_weight_ref,
    key_copy_ref,
    update_ref,
):
    core, half, row = place_ref[0], place_ref[1], place_ref[2]
    rows, _, count, width = ratio_ref.shape
    own_rows = query_step_ref.shape[0]
    ranks = rows * count
    outs = (
        (query_master_ref, query_step_ref, query_weight_ref, query_copy_ref),
        (key_master_ref, key_step_ref, key_weight_ref, key_copy_ref),
    )

    def whole(first_ref, second_ref, k):
        upto = rows // 2
        first = ratio_ref[pl.ds(half * upto, upto), k].reshape(ranks // 2, width)
        second = ratio_ref[pl.ds((1 - half) * upto, upto), k].reshape(ranks // 2, width)

        def some(i, total):
            span = pl.ds(pl.multiple_of(i * BLOCK, BLOCK), BLOCK)
            update = jnp.dot(first_ref[span, :], first, preferred_element_type=F32)
            update += jnp.dot(second_ref[span, :], second, preferred_element_type=F32)
            update_ref[k, span, :] = update
            return total + jnp.sum((update * update).reshape(BLOCK // 8, 8, width), axis=0)

        return lax.fori_loop(0, D // BLOCK, some, jnp.zeros((8, width), F32))

    for k in range(2):
        total = lax.cond(
            core == k,
            lambda: whole(own_a_ref, own_b_ref, k),
            lambda: whole(other_a_ref, other_b_ref, k),
        )
        scale = 1.0 / jnp.sqrt(jnp.sum(total, keepdims=True) / (D * HD) + norm_floor)
        master_ref, step_ref, weight_ref, copy_ref = outs[k]

        def some(i, carry):
            span = pl.ds(pl.multiple_of(i * own_rows, own_rows), own_rows)
            step = update_ref[k, span, :] * scale
            copy_ref[span, :] = (masters_ref[i, k].astype(F32) - step_rate * step).astype(BF)
            return carry

        lax.fori_loop(0, D // own_rows, some, 0)
        span = pl.ds(pl.multiple_of(row * own_rows, own_rows), own_rows)
        step = update_ref[k, span, :] * scale
        step_ref[...] = step
        weight_ref[...] = master_ref[...] - step_rate * step


def finish(place, ratio, own_a, own_b, other_a, other_b, masters, query_master, key_master):
    own_rows, width = query_master.shape
    mine = jax.ShapeDtypeStruct((own_rows, width), F32)
    copied = jax.ShapeDtypeStruct((D, width), BF)
    return pl.pallas_call(
        finish_kernel,
        out_shape=(mine, mine, copied) * 2,
        in_specs=[pl.BlockSpec(memory_space=pltpu.SMEM)] + [pl.BlockSpec(memory_space=pltpu.VMEM)] * 8,
        scratch_shapes=[pltpu.VMEM((2, D, width), F32)],
        compiler_params=VMEM,
        name="finish",
    )(place, ratio, own_a, own_b, other_a, other_b, masters, query_master, key_master)


def body(
    saved_input,
    query_cot,
    key_cot,
    query_master,
    key_master,
    query_basis,
    key_basis,
    query_first,
    query_second,
    key_first,
    key_second,
):
    rows = lax.axis_size(FS)
    depth = lax.axis_size("z")
    tokens, width = query_cot.shape
    low_count = query_first.shape[0]
    ranks = query_basis.shape[1]
    pairs = depth // 2
    share = tokens // pairs
    core = lax.axis_index("c")
    half = lax.axis_index("z") % 2
    place = jnp.stack([core, half, lax.axis_index(FS)]).astype(jnp.int32)
    first_core = core == 0

    pieces = saved_input.reshape(pairs, 1, share, width)
    pieces = jnp.broadcast_to(pieces, (pairs, 2, share, width)).reshape(depth, share, width)
    pieces = lax.all_to_all(pieces, "z", 0, 0, tiled=True)
    own_basis = jnp.where(first_core, query_basis, key_basis)
    own_half = jnp.where(half == 0, own_basis[:, : ranks // 2], own_basis[:, ranks // 2 :])
    basis = sent_to_all(own_half, FS)
    other_pieces = swapped(pieces, "c")
    own_cot = jnp.where(first_core, query_cot, key_cot)
    other_cot = swapped(jnp.where(first_core, key_cot, query_cot), "c")
    low = product(place, pieces, other_pieces, basis)
    low = lax.all_gather(low, "z", axis=0, tiled=True)
    low = low.reshape(pairs, 2, share, ranks // 2)
    masters = sent_to_all(jnp.stack([query_master, key_master]).astype(BF), FS)

    partial = partials(place, low, own_cot, other_cot, rows, low_count)
    partial = partial.reshape(2 * rows, low_count, width)
    partial = lax.all_to_all(partial, (*FS, "c"), 0, 0, tiled=True)
    projected = jnp.sum(partial.reshape(rows, 2, low_count, width).astype(F32), axis=0)
    firsts = jnp.stack([query_first, key_first])
    seconds = jnp.stack([query_second, key_second])
    first_new = moment_decay * firsts + (1.0 - moment_decay) * projected
    second_new = square_decay * seconds + (1.0 - square_decay) * projected * projected
    ratio = (first_new / jnp.sqrt(second_new + square_floor)).astype(BF)
    ratio = sent_to_all(ratio, FS).reshape(rows, 2, low_count, width)

    basis = basis.reshape(D, ranks // 2)
    pair_basis = swapped(basis, "z")
    other_basis = swapped(basis, "c")
    other_pair_basis = swapped(pair_basis, "c")
    query_step, query_weight, query_copy, key_step, key_weight, key_copy = finish(
        place,
        ratio,
        basis,
        pair_basis,
        other_basis,
        other_pair_basis,
        masters.reshape(rows, 2, -1, width),
        query_master,
        key_master,
    )
    return (
        query_step,
        query_weight,
        query_copy,
        first_new[0],
        second_new[0],
        key_step,
        key_weight,
        key_copy,
        first_new[1],
        second_new[1],
    )


def solution(mesh):
    torus = Mesh(mesh.devices.reshape(4, 4, 16, 2), ("y", "x", "z", "c"))
    tp = ("z", "c")
    split = P(FS, tp)
    rows = P(FS, None)
    copied = P(None, tp)
    in_specs = (split,) * 5 + (rows,) * 2 + (split,) * 4
    out_specs = (split, split, copied, split, split) * 2

    return jax.shard_map(body, mesh=torus, in_specs=in_specs, out_specs=out_specs, check_vma=False)
```

```python
import jax
import jax.numpy as jnp
from jax import lax
from jax.experimental import pallas as pl
from jax.experimental.pallas import tpu as pltpu
from jax.sharding import Mesh
from jax.sharding import PartitionSpec as P


D = 4096
HD = 128
FS = ("y", "x")
BF = jnp.bfloat16
F32 = jnp.float32

moment_decay = 0.8
square_decay = 0.9
square_floor = 1.0
norm_floor = 0.01
step_rate = 0.01

VMEM = pltpu.CompilerParams(vmem_limit_bytes=48 * 1024 * 1024)


def sent_to_all(x, axis):
    count = lax.axis_size(axis)
    return lax.all_to_all(jnp.broadcast_to(x[None], (count, *x.shape)), axis, 0, 0, tiled=True)


def swapped(x, axis):
    count = lax.axis_size(axis)
    return lax.ppermute(x, axis, [(i, i ^ 1) for i in range(count)])


def product_kernel(core_ref, own_ref, other_ref, top_ref, rest_ref, out_ref):
    core = core_ref[0]
    cut = top_ref.shape[1]
    first = core == 0

    def some(z, total):
        own, other = own_ref[z], other_ref[z]
        left = jnp.where(first, own, other)
        right = jnp.where(first, other, own)
        total += jnp.dot(left[:, :cut], top_ref[z], preferred_element_type=F32)
        both = jnp.concatenate([left[:, cut:], right], axis=1)
        return total + jnp.dot(both, rest_ref[z], preferred_element_type=F32)

    total = lax.fori_loop(0, own_ref.shape[0], some, jnp.zeros(out_ref.shape, F32), unroll=4)
    out_ref[...] = total.astype(out_ref.dtype)


def product(core, own, other, top, rest):
    return pl.pallas_call(
        product_kernel,
        out_shape=jax.ShapeDtypeStruct((own.shape[1], top.shape[-1]), BF),
        in_specs=[pl.BlockSpec(memory_space=pltpu.SMEM)] + [pl.BlockSpec(memory_space=pltpu.VMEM)] * 4,
        compiler_params=VMEM,
        name="product",
    )(core, own, other, top, rest)


def partial_kernel(core_ref, low_ref, own_ref, other_ref, out_ref):
    core = core_ref[0]
    rows, _, count, width = out_ref.shape
    contract = (((0,), (0,)), ((), ()))
    mine = lax.dot_general(low_ref[...], own_ref[...], contract, preferred_element_type=F32)
    theirs = lax.dot_general(low_ref[...], other_ref[...], contract, preferred_element_type=F32)
    out_ref[:, core] = mine.reshape(rows, count, width).astype(out_ref.dtype)
    out_ref[:, 1 - core] = theirs.reshape(rows, count, width).astype(out_ref.dtype)


def partials(core, low, own, other, rows, count):
    return pl.pallas_call(
        partial_kernel,
        out_shape=jax.ShapeDtypeStruct((rows, 2, count, own.shape[-1]), BF),
        in_specs=[pl.BlockSpec(memory_space=pltpu.SMEM)] + [pl.BlockSpec(memory_space=pltpu.VMEM)] * 3,
        compiler_params=VMEM,
        name="partials",
    )(core, low, own, other)


GROUP = 4


def finish_kernel(
    place_ref,
    ratio_ref,
    own_top_ref,
    own_rest_ref,
    other_top_hbm,
    other_rest_hbm,
    masters_hbm,
    query_master_ref,
    key_master_ref,
    query_step_ref,
    query_weight_ref,
    query_copy_hbm,
    key_step_ref,
    key_weight_ref,
    key_copy_hbm,
    other_top_ref,
    other_rest_ref,
    masters_ref,
    update_top_ref,
    update_rest_ref,
    copies_ref,
    scales_ref,
    arrived,
    left,
):
    core, row = place_ref[0], place_ref[1]
    rows, _, count, width = ratio_ref.shape
    ranks = rows * count
    top, rest = own_top_ref.shape[1], own_rest_ref.shape[1]
    tops, rests = pl.ds(0, top), pl.ds(top, rest)
    incoming = [
        pltpu.make_async_copy(other_top_hbm, other_top_ref, arrived.at[0]),
        pltpu.make_async_copy(other_rest_hbm, other_rest_ref, arrived.at[1]),
        pltpu.make_async_copy(masters_hbm, masters_ref, arrived.at[2]),
    ]
    outgoing = [
        pltpu.make_async_copy(copies_ref.at[0], query_copy_hbm, left.at[0]),
        pltpu.make_async_copy(copies_ref.at[1], key_copy_hbm, left.at[1]),
    ]
    for copy in incoming:
        copy.start()

    def whole(top_ref, rest_ref, k):
        ratio = ratio_ref[:, k].reshape(ranks, width)

        def some(i, total):
            span = pl.ds(i * GROUP, GROUP)
            for part_ref, update_ref, size in ((top_ref, update_top_ref, top), (rest_ref, update_rest_ref, rest)):
                part = part_ref[span].reshape(GROUP * size, ranks)
                update = jnp.dot(part, ratio, preferred_element_type=F32)
                update_ref[k, span] = update.reshape(GROUP, size, width)
                total += jnp.sum((update * update).reshape(GROUP * size // 8, 8, width), axis=0)
            return total

        total = lax.fori_loop(0, rows // GROUP, some, jnp.zeros((8, width), F32))
        scale = 1.0 / jnp.sqrt(jnp.sum(total, keepdims=True) / (D * HD) + norm_floor)
        scales_ref[k] = jnp.broadcast_to(scale, (8, width))

    def copied(k):
        scale = scales_ref[k][:1]

        def some(f, carry):
            step = update_top_ref[k, f] * scale
            copies_ref[k, f, tops, :] = (masters_ref[f, k, tops, :].astype(F32) - step_rate * step).astype(BF)
            step = update_rest_ref[k, f] * scale
            copies_ref[k, f, rests, :] = (masters_ref[f, k, rests, :].astype(F32) - step_rate * step).astype(BF)
            return carry

        lax.fori_loop(0, rows, some, 0)
        for n in range(2):
            pl.when(k == n)(outgoing[n].start)

    whole(own_top_ref, own_rest_ref, core)
    incoming[2].wait()
    copied(core)
    incoming[0].wait()
    incoming[1].wait()
    whole(other_top_ref, other_rest_ref, 1 - core)
    copied(1 - core)
    outs = (
        (query_master_ref, query_step_ref, query_weight_ref),
        (key_master_ref, key_step_ref, key_weight_ref),
    )
    for k, (master_ref, step_ref, weight_ref) in enumerate(outs):
        scale = scales_ref[k][:1]
        for span, update_ref in ((tops, update_top_ref), (rests, update_rest_ref)):
            step = update_ref[k, row] * scale
            step_ref[span, :] = step
            weight_ref[span, :] = master_ref[span, :] - step_rate * step
    for copy in outgoing:
        copy.wait()


def finish(place, ratio, own_top, own_rest, other_top, other_rest, masters, query_master, key_master):
    own_rows, width = query_master.shape
    rows = ratio.shape[0]
    top, rest = own_top.shape[1], own_rest.shape[1]
    mine = jax.ShapeDtypeStruct((own_rows, width), F32)
    copied = jax.ShapeDtypeStruct((rows, own_rows, width), BF)
    smem, vmem, anywhere = (
        pl.BlockSpec(memory_space=pltpu.SMEM),
        pl.BlockSpec(memory_space=pltpu.VMEM),
        pl.BlockSpec(memory_space=pl.ANY),
    )
    return pl.pallas_call(
        finish_kernel,
        out_shape=(mine, mine, copied) * 2,
        in_specs=[smem, vmem, vmem, vmem, anywhere, anywhere, anywhere, vmem, vmem],
        out_specs=(vmem, vmem, anywhere) * 2,
        scratch_shapes=[
            pltpu.VMEM(other_top.shape, BF),
            pltpu.VMEM(other_rest.shape, BF),
            pltpu.VMEM(masters.shape, BF),
            pltpu.VMEM((2, rows, top, width), F32),
            pltpu.VMEM((2, rows, rest, width), F32),
            pltpu.VMEM((2, rows, own_rows, width), BF),
            pltpu.VMEM((2, 8, width), F32),
            pltpu.SemaphoreType.DMA((3,)),
            pltpu.SemaphoreType.DMA((2,)),
        ],
        compiler_params=VMEM,
        name="finish",
    )(place, ratio, own_top, own_rest, other_top, other_rest, masters, query_master, key_master)


TOP = 112


def body(
    saved_input,
    query_cot,
    key_cot,
    query_master,
    key_master,
    query_basis,
    key_basis,
    query_first,
    query_second,
    key_first,
    key_second,
):
    rows = lax.axis_size(FS)
    depth = lax.axis_size("z")
    tokens, width = query_cot.shape
    low_count = query_first.shape[0]
    ranks = query_basis.shape[1]
    share = tokens // depth
    core = lax.axis_index("c")
    place = jnp.stack([core, lax.axis_index(FS)]).astype(jnp.int32)
    first_core = core == 0

    pieces = lax.all_to_all(saved_input.reshape(depth, share, width), "z", 0, 0, tiled=True)
    own_basis = jnp.where(first_core, query_basis, key_basis)
    top = lax.all_gather(own_basis[:TOP], FS, axis=0, tiled=True).reshape(rows, TOP, ranks)
    rest = sent_to_all(own_basis[TOP:], FS)
    rest = rest.reshape(rows, -1, ranks)
    other_pieces = swapped(pieces, "c")
    own_cot = jnp.where(first_core, query_cot, key_cot)
    other_cot = swapped(jnp.where(first_core, key_cot, query_cot), "c")
    low = product(place, pieces, other_pieces, top, rest)
    low = lax.all_gather(low, "z", axis=0, tiled=True)
    masters = sent_to_all(jnp.stack([query_master, key_master]).astype(BF), FS)

    partial = partials(place, low, own_cot, other_cot, rows, low_count)
    partial = partial.reshape(2 * rows, low_count, width)
    partial = lax.all_to_all(partial, (*FS, "c"), 0, 0, tiled=True)
    projected = jnp.sum(partial.reshape(rows, 2, low_count, width).astype(F32), axis=0)
    firsts = jnp.stack([query_first, key_first])
    seconds = jnp.stack([query_second, key_second])
    first_new = moment_decay * firsts + (1.0 - moment_decay) * projected
    second_new = square_decay * seconds + (1.0 - square_decay) * projected * projected
    ratio = (first_new / jnp.sqrt(second_new + square_floor)).astype(BF)
    ratio = sent_to_all(ratio, FS).reshape(rows, 2, low_count, width)

    other_top = swapped(top, "c")
    other_rest = swapped(rest, "c")
    query_step, query_weight, query_copy, key_step, key_weight, key_copy = finish(
        place,
        ratio,
        top,
        rest,
        other_top,
        other_rest,
        masters.reshape(rows, 2, -1, width),
        query_master,
        key_master,
    )
    return (
        query_step,
        query_weight,
        query_copy.reshape(D, width),
        first_new[0],
        second_new[0],
        key_step,
        key_weight,
        key_copy.reshape(D, width),
        first_new[1],
        second_new[1],
    )


def solution(mesh):
    torus = Mesh(mesh.devices.reshape(4, 4, 16, 2), ("y", "x", "z", "c"))
    tp = ("z", "c")
    split = P(FS, tp)
    rows = P(FS, None)
    copied = P(None, tp)
    in_specs = (split,) * 5 + (rows,) * 2 + (split,) * 4
    out_specs = (split, split, copied, split, split) * 2

    return jax.shard_map(body, mesh=torus, in_specs=in_specs, out_specs=out_specs, check_vma=False)
```

```python
import jax
import jax.numpy as jnp
from jax import lax
from jax.experimental import pallas as pl
from jax.experimental.pallas import tpu as pltpu
from jax.sharding import Mesh
from jax.sharding import PartitionSpec as P


D = 4096
HD = 128
FS = ("y", "x")
BF = jnp.bfloat16
F32 = jnp.float32

moment_decay = 0.8
square_decay = 0.9
square_floor = 1.0
norm_floor = 0.01
step_rate = 0.01

VMEM = pltpu.CompilerParams(vmem_limit_bytes=48 * 1024 * 1024)


def sent_to_all(x, axis):
    count = lax.axis_size(axis)
    return lax.all_to_all(jnp.broadcast_to(x[None], (count, *x.shape)), axis, 0, 0, tiled=True)


def swapped(x, axis):
    count = lax.axis_size(axis)
    return lax.ppermute(x, axis, [(i, i ^ 1) for i in range(count)])


def product_kernel(own_ref, other_ref, top_ref, rest_ref, out_ref):
    core = lax.axis_index("c")
    cut = top_ref.shape[1]
    first = core == 0

    def some(z, total):
        own, other = own_ref[z], other_ref[z]
        left = jnp.where(first, own, other)
        right = jnp.where(first, other, own)
        total += jnp.dot(left[:, :cut], top_ref[z], preferred_element_type=F32)
        both = jnp.concatenate([left[:, cut:], right], axis=1)
        return total + jnp.dot(both, rest_ref[z], preferred_element_type=F32)

    total = lax.fori_loop(0, own_ref.shape[0], some, jnp.zeros(out_ref.shape, F32), unroll=4)
    out_ref[...] = total.astype(out_ref.dtype)


def product(own, other, top, rest):
    return pl.pallas_call(
        product_kernel,
        out_shape=jax.ShapeDtypeStruct((own.shape[1], top.shape[-1]), BF),
        in_specs=[pl.BlockSpec(memory_space=pltpu.VMEM)] * 4,
        compiler_params=VMEM,
        name="product",
    )(own, other, top, rest)


def partial_kernel(low_ref, own_ref, other_ref, out_ref):
    core = lax.axis_index("c")
    rows, _, count, width = out_ref.shape
    contract = (((0,), (0,)), ((), ()))
    cots = jnp.concatenate([own_ref[...], other_ref[...]], axis=1)
    both = lax.dot_general(low_ref[...], cots, contract, preferred_element_type=F32).astype(out_ref.dtype)
    out_ref[:, core] = both[:, :width].reshape(rows, count, width)
    out_ref[:, 1 - core] = both[:, width:].reshape(rows, count, width)


def partials(low, own, other, rows, count):
    return pl.pallas_call(
        partial_kernel,
        out_shape=jax.ShapeDtypeStruct((rows, 2, count, own.shape[-1]), BF),
        in_specs=[pl.BlockSpec(memory_space=pltpu.VMEM)] * 3,
        compiler_params=VMEM,
        name="partials",
    )(low, own, other)


def moments_kernel(
    parts_ref,
    query_first_hbm,
    query_second_hbm,
    key_first_hbm,
    key_second_hbm,
    query_first_new_ref,
    query_second_new_ref,
    key_first_new_ref,
    key_second_new_ref,
    ratio_ref,
    olds_ref,
    arrived,
):
    rows = ratio_ref.shape[0]
    outs = ((query_first_new_ref, query_second_new_ref), (key_first_new_ref, key_second_new_ref))
    olds = (query_first_hbm, query_second_hbm, key_first_hbm, key_second_hbm)
    incoming = [pltpu.make_async_copy(old, olds_ref.at[n], arrived.at[n]) for n, old in enumerate(olds)]
    for copy in incoming:
        copy.start()
    sums = []
    for k in range(2):
        projected = parts_ref[k].astype(F32)
        for f in range(1, rows):
            projected += parts_ref[2 * f + k].astype(F32)
        sums.append(projected)
    for copy in incoming:
        copy.wait()
    for k, projected in enumerate(sums):
        first_new = moment_decay * olds_ref[2 * k] + (1.0 - moment_decay) * projected
        second_new = square_decay * olds_ref[2 * k + 1] + (1.0 - square_decay) * projected * projected
        outs[k][0][...] = first_new
        outs[k][1][...] = second_new
        ratio = (first_new / jnp.sqrt(second_new + square_floor)).astype(BF)
        for f in range(rows):
            ratio_ref[f, k] = ratio


def moments(parts, query_first, query_second, key_first, key_second):
    count, width = query_first.shape
    own = jax.ShapeDtypeStruct((count, width), F32)
    ratios = jax.ShapeDtypeStruct((parts.shape[0] // 2, 2, count, width), BF)
    return pl.pallas_call(
        moments_kernel,
        out_shape=(own, own, own, own, ratios),
        in_specs=[pl.BlockSpec(memory_space=pltpu.VMEM)] + [pl.BlockSpec(memory_space=pl.ANY)] * 4,
        scratch_shapes=[pltpu.VMEM((4, count, width), F32), pltpu.SemaphoreType.DMA((4,))],
        compiler_params=VMEM,
        name="moments",
    )(parts, query_first, query_second, key_first, key_second)


GROUP = 4


def finish_kernel(
    ratio_ref,
    own_top_ref,
    own_rest_ref,
    other_top_hbm,
    other_rest_hbm,
    masters_hbm,
    query_master_ref,
    key_master_ref,
    query_step_ref,
    query_weight_ref,
    query_copy_hbm,
    key_step_ref,
    key_weight_ref,
    key_copy_hbm,
    other_top_ref,
    other_rest_ref,
    masters_ref,
    update_top_ref,
    update_rest_ref,
    copies_ref,
    scales_ref,
    arrived,
    left,
):
    core, row = lax.axis_index("c"), lax.axis_index(FS)
    rows, _, count, width = ratio_ref.shape
    ranks = rows * count
    top, rest = own_top_ref.shape[1], own_rest_ref.shape[1]
    tops, rests = pl.ds(0, top), pl.ds(top, rest)
    incoming = [
        pltpu.make_async_copy(other_top_hbm, other_top_ref, arrived.at[0]),
        pltpu.make_async_copy(other_rest_hbm, other_rest_ref, arrived.at[1]),
        pltpu.make_async_copy(masters_hbm, masters_ref, arrived.at[2]),
    ]
    copy_hbms = (query_copy_hbm, key_copy_hbm)

    def leaving(k, part):
        span = pl.ds(part * GROUP, GROUP)
        return pltpu.make_async_copy(copies_ref.at[k, span], copy_hbms[k].at[span], left.at[k, part])

    for copy in incoming:
        copy.start()

    def products(top_ref, rest_ref, k, ratio, part, total):
        span = pl.ds(part * GROUP, GROUP)
        for basis_ref, update_ref, size in ((top_ref, update_top_ref, top), (rest_ref, update_rest_ref, rest)):
            basis = basis_ref[span].reshape(GROUP * size, ranks)
            update = jnp.dot(basis, ratio, preferred_element_type=F32)
            update_ref[k, span] = update.reshape(GROUP, size, width)
            total += jnp.sum((update * update).reshape(GROUP * size // 8, 8, width), axis=0)
        return total

    def scaled(k, total):
        scale = 1.0 / jnp.sqrt(jnp.sum(total, keepdims=True) / (D * HD) + norm_floor)
        scales_ref[k] = jnp.broadcast_to(scale, (8, width))

    def copied(k, part):
        scale = scales_ref[k][:1]
        for n in range(GROUP):
            f = part * GROUP + n
            for span, update_ref in ((tops, update_top_ref), (rests, update_rest_ref)):
                step = update_ref[k, f] * scale
                copies_ref[k, f, span, :] = (masters_ref[f, k, span, :].astype(F32) - step_rate * step).astype(BF)

    def sent(k, part):
        for n in range(2):
            pl.when(k == n)(leaving(n, part).start)

    parts = rows // GROUP
    mine, theirs = core, 1 - core
    ratio = ratio_ref[:, mine].reshape(ranks, width)
    total = jnp.zeros((8, width), F32)
    for part in range(parts):
        total = products(own_top_ref, own_rest_ref, mine, ratio, part, total)
    scaled(mine, total)
    for copy in incoming:
        copy.wait()
    ratio = ratio_ref[:, theirs].reshape(ranks, width)
    total = jnp.zeros((8, width), F32)
    for part in range(parts):
        total = products(other_top_ref, other_rest_ref, theirs, ratio, part, total)
        copied(mine, part)
        sent(mine, part)
    scaled(theirs, total)
    for part in range(parts):
        copied(theirs, part)
        sent(theirs, part)
    outs = (
        (query_master_ref, query_step_ref, query_weight_ref),
        (key_master_ref, key_step_ref, key_weight_ref),
    )
    for k, (master_ref, step_ref, weight_ref) in enumerate(outs):
        scale = scales_ref[k][:1]
        for span, update_ref in ((tops, update_top_ref), (rests, update_rest_ref)):
            step = update_ref[k, row] * scale
            step_ref[span, :] = step
            weight_ref[span, :] = master_ref[span, :] - step_rate * step
    for k in range(2):
        for part in range(parts):
            leaving(k, part).wait()


def finish(ratio, own_top, own_rest, other_top, other_rest, masters, query_master, key_master):
    own_rows, width = query_master.shape
    rows = ratio.shape[0]
    top, rest = own_top.shape[1], own_rest.shape[1]
    mine = jax.ShapeDtypeStruct((own_rows, width), F32)
    copied = jax.ShapeDtypeStruct((rows, own_rows, width), BF)
    vmem, anywhere = pl.BlockSpec(memory_space=pltpu.VMEM), pl.BlockSpec(memory_space=pl.ANY)
    return pl.pallas_call(
        finish_kernel,
        out_shape=(mine, mine, copied) * 2,
        in_specs=[vmem, vmem, vmem, anywhere, anywhere, anywhere, vmem, vmem],
        out_specs=(vmem, vmem, anywhere) * 2,
        scratch_shapes=[
            pltpu.VMEM(other_top.shape, BF),
            pltpu.VMEM(other_rest.shape, BF),
            pltpu.VMEM(masters.shape, BF),
            pltpu.VMEM((2, rows, top, width), F32),
            pltpu.VMEM((2, rows, rest, width), F32),
            pltpu.VMEM((2, rows, own_rows, width), BF),
            pltpu.VMEM((2, 8, width), F32),
            pltpu.SemaphoreType.DMA((3,)),
            pltpu.SemaphoreType.DMA((2, rows // GROUP)),
        ],
        compiler_params=VMEM,
        name="finish",
    )(ratio, own_top, own_rest, other_top, other_rest, masters, query_master, key_master)


TOP = 112


def body(
    saved_input,
    query_cot,
    key_cot,
    query_master,
    key_master,
    query_basis,
    key_basis,
    query_first,
    query_second,
    key_first,
    key_second,
):
    rows = lax.axis_size(FS)
    depth = lax.axis_size("z")
    tokens, width = query_cot.shape
    low_count = query_first.shape[0]
    ranks = query_basis.shape[1]
    share = tokens // depth
    core = lax.axis_index("c")
    first_core = core == 0

    pieces = lax.all_to_all(saved_input.reshape(depth, share, width), "z", 0, 0, tiled=True)
    own_basis = jnp.where(first_core, query_basis, key_basis)
    top = lax.all_gather(own_basis[:TOP], FS, axis=0, tiled=True).reshape(rows, TOP, ranks)
    rest = sent_to_all(own_basis[TOP:], FS)
    rest = rest.reshape(rows, -1, ranks)
    other_pieces = swapped(pieces, "c")
    own_cot = jnp.where(first_core, query_cot, key_cot)
    other_cot = swapped(jnp.where(first_core, key_cot, query_cot), "c")
    low = product(pieces, other_pieces, top, rest)
    low = lax.all_gather(low, "z", axis=0, tiled=True)
    masters = sent_to_all(jnp.stack([query_master, key_master]).astype(BF), FS)

    partial = partials(low, own_cot, other_cot, rows, low_count)
    partial = partial.reshape(2 * rows, low_count, width)
    partial = lax.all_to_all(partial, (*FS, "c"), 0, 0, tiled=True)
    *news, ratio = moments(partial, query_first, query_second, key_first, key_second)
    ratio = lax.all_to_all(ratio, FS, 0, 0, tiled=True)

    other_top = swapped(top, "c")
    other_rest = swapped(rest, "c")
    query_step, query_weight, query_copy, key_step, key_weight, key_copy = finish(
        ratio,
        top,
        rest,
        other_top,
        other_rest,
        masters.reshape(rows, 2, -1, width),
        query_master,
        key_master,
    )
    return (
        query_step,
        query_weight,
        query_copy.reshape(D, width),
        news[0],
        news[1],
        key_step,
        key_weight,
        key_copy.reshape(D, width),
        news[2],
        news[3],
    )


def solution(mesh):
    torus = Mesh(mesh.devices.reshape(4, 4, 16, 2), ("y", "x", "z", "c"))
    tp = ("z", "c")
    split = P(FS, tp)
    rows = P(FS, None)
    copied = P(None, tp)
    in_specs = (split,) * 5 + (rows,) * 2 + (split,) * 4
    out_specs = (split, split, copied, split, split) * 2

    return jax.shard_map(body, mesh=torus, in_specs=in_specs, out_specs=out_specs, check_vma=False)
```

```python
import jax
import jax.numpy as jnp
from jax import lax
from jax.experimental import pallas as pl
from jax.experimental.pallas import tpu as pltpu
from jax.sharding import Mesh
from jax.sharding import PartitionSpec as P


D = 4096
HD = 128
FS = ("y", "x")
BF = jnp.bfloat16
F32 = jnp.float32

moment_decay = 0.8
square_decay = 0.9
square_floor = 1.0
norm_floor = 0.01
step_rate = 0.01

VMEM = pltpu.CompilerParams(vmem_limit_bytes=48 * 1024 * 1024)


def swapped(x, axis):
    count = lax.axis_size(axis)
    return lax.ppermute(x, axis, [(i, i ^ 1) for i in range(count)])


def product_kernel(pieces_ref, basis_ref, out_ref):
    groups, chips, share, width = pieces_ref.shape
    ranks = out_ref.shape[-1]
    total = jnp.zeros((groups * share, 2 * ranks), F32)
    for z in range(chips):
        piece = pieces_ref[:, z].reshape(groups * share, width)
        total += jnp.dot(piece, basis_ref[z], preferred_element_type=F32)
    total = total.astype(BF)
    for c in range(2):
        out_ref[:, c] = total[:, c * ranks : (c + 1) * ranks].reshape(groups, share, ranks)


def product(pieces, basis):
    groups, _, share, _ = pieces.shape
    return pl.pallas_call(
        product_kernel,
        out_shape=jax.ShapeDtypeStruct((groups, 2, share, basis.shape[-1] // 2), BF),
        in_specs=[pl.BlockSpec(memory_space=pltpu.VMEM)] * 2,
        compiler_params=VMEM,
        name="product",
    )(pieces, basis)


def total_kernel(parts_ref, out_ref):
    total = parts_ref[0].astype(F32)
    for n in range(1, parts_ref.shape[0]):
        total += parts_ref[n].astype(F32)
    total = total.astype(BF)
    for n in range(out_ref.shape[0]):
        out_ref[n] = total


def totals(parts, copies):
    return pl.pallas_call(
        total_kernel,
        out_shape=jax.ShapeDtypeStruct((copies, *parts.shape[1:]), BF),
        in_specs=[pl.BlockSpec(memory_space=pltpu.VMEM)],
        compiler_params=VMEM,
        name="totals",
    )(parts)


def partial_kernel(low_ref, own_ref, other_ref, out_ref):
    core = lax.axis_index("c")
    rows, _, count, width = out_ref.shape
    contract = (((0,), (0,)), ((), ()))
    cots = jnp.concatenate([own_ref[...], other_ref[...]], axis=1)
    both = lax.dot_general(low_ref[...], cots, contract, preferred_element_type=F32).astype(out_ref.dtype)
    out_ref[:, core] = both[:, :width].reshape(rows, count, width)
    out_ref[:, 1 - core] = both[:, width:].reshape(rows, count, width)


def partials(low, own, other, rows, count):
    return pl.pallas_call(
        partial_kernel,
        out_shape=jax.ShapeDtypeStruct((rows, 2, count, own.shape[-1]), BF),
        in_specs=[pl.BlockSpec(memory_space=pltpu.VMEM)] * 3,
        compiler_params=VMEM,
        name="partials",
    )(low, own, other)


def moments_kernel(
    parts_ref,
    query_first_hbm,
    query_second_hbm,
    key_first_hbm,
    key_second_hbm,
    query_first_new_ref,
    query_second_new_ref,
    key_first_new_ref,
    key_second_new_ref,
    ratio_ref,
    olds_ref,
    arrived,
):
    rows = ratio_ref.shape[0]
    outs = ((query_first_new_ref, query_second_new_ref), (key_first_new_ref, key_second_new_ref))
    olds = (query_first_hbm, query_second_hbm, key_first_hbm, key_second_hbm)
    incoming = [pltpu.make_async_copy(old, olds_ref.at[n], arrived.at[n]) for n, old in enumerate(olds)]
    for copy in incoming:
        copy.start()
    sums = []
    for k in range(2):
        projected = parts_ref[k].astype(F32)
        for f in range(1, rows):
            projected += parts_ref[2 * f + k].astype(F32)
        sums.append(projected)
    for copy in incoming:
        copy.wait()
    for k, projected in enumerate(sums):
        first_new = moment_decay * olds_ref[2 * k] + (1.0 - moment_decay) * projected
        second_new = square_decay * olds_ref[2 * k + 1] + (1.0 - square_decay) * projected * projected
        outs[k][0][...] = first_new
        outs[k][1][...] = second_new
        ratio = (first_new / jnp.sqrt(second_new + square_floor)).astype(BF)
        for f in range(rows):
            ratio_ref[f, k] = ratio


def moments(parts, query_first, query_second, key_first, key_second):
    count, width = query_first.shape
    own = jax.ShapeDtypeStruct((count, width), F32)
    ratios = jax.ShapeDtypeStruct((parts.shape[0] // 2, 2, count, width), BF)
    return pl.pallas_call(
        moments_kernel,
        out_shape=(own, own, own, own, ratios),
        in_specs=[pl.BlockSpec(memory_space=pltpu.VMEM)] + [pl.BlockSpec(memory_space=pltpu.HBM)] * 4,
        scratch_shapes=[pltpu.VMEM((4, count, width), F32), pltpu.SemaphoreType.DMA((4,))],
        compiler_params=VMEM,
        name="moments",
    )(parts, query_first, query_second, key_first, key_second)


GROUP = 4


def finish_kernel(
    ratio_ref,
    own_ref,
    other_hbm,
    bulk_hbm,
    query_master_ref,
    key_master_ref,
    query_step_ref,
    query_weight_ref,
    query_copy_hbm,
    key_step_ref,
    key_weight_ref,
    key_copy_hbm,
    other_ref,
    masters_ref,
    update_ref,
    copies_ref,
    scales_ref,
    arrived,
    left,
):
    core, row = lax.axis_index("c"), lax.axis_index(FS)
    rows, _, _, width = ratio_ref.shape
    own_rows, ranks = own_ref.shape[2], 2 * own_ref.shape[3]
    incoming = [
        pltpu.make_async_copy(other_hbm, other_ref, arrived.at[0]),
        pltpu.make_async_copy(bulk_hbm.at[:, pl.ds(2, 2)], masters_ref, arrived.at[1]),
    ]
    copy_hbms = (query_copy_hbm, key_copy_hbm)

    def leaving(k, part):
        span = pl.ds(part * GROUP, GROUP)
        return pltpu.make_async_copy(copies_ref.at[k, span], copy_hbms[k].at[span], left.at[k, part])

    for copy in incoming:
        copy.start()

    def products(basis_ref, k, ratio, part, total):
        span = pl.ds(part * GROUP, GROUP)
        update = jnp.zeros((GROUP * own_rows, width), F32)
        for n in range(2):
            basis = basis_ref[span, n].reshape(GROUP * own_rows, ranks // 2)
            update += jnp.dot(basis, ratio[n * ranks // 2 : (n + 1) * ranks // 2], preferred_element_type=F32)
        update_ref[k, span] = update.reshape(GROUP, own_rows, width)
        return total + jnp.sum((update * update).reshape(GROUP * own_rows // 8, 8, width), axis=0)

    def scaled(k, total):
        scale = 1.0 / jnp.sqrt(jnp.sum(total, keepdims=True) / (D * HD) + norm_floor)
        scales_ref[k] = jnp.broadcast_to(scale, (8, width))

    def copied(k, part):
        scale = scales_ref[k][:1]
        for n in range(GROUP):
            f = part * GROUP + n
            step = update_ref[k, f] * scale
            copies_ref[k, f] = (masters_ref[f, k].astype(F32) - step_rate * step).astype(BF)

    def sent(k, part):
        for n in range(2):
            pl.when(k == n)(leaving(n, part).start)

    parts = rows // GROUP
    mine, theirs = core, 1 - core
    ratio = ratio_ref[:, mine].reshape(ranks, width)
    total = jnp.zeros((8, width), F32)
    for part in range(parts):
        total = products(own_ref, mine, ratio, part, total)
    scaled(mine, total)
    for copy in incoming:
        copy.wait()
    ratio = ratio_ref[:, theirs].reshape(ranks, width)
    total = jnp.zeros((8, width), F32)
    for part in range(parts):
        total = products(other_ref, theirs, ratio, part, total)
        copied(mine, part)
        sent(mine, part)
    scaled(theirs, total)
    for part in range(parts):
        copied(theirs, part)
        sent(theirs, part)
    outs = (
        (query_master_ref, query_step_ref, query_weight_ref),
        (key_master_ref, key_step_ref, key_weight_ref),
    )
    for k, (master_ref, step_ref, weight_ref) in enumerate(outs):
        scale = scales_ref[k][:1]
        step = update_ref[k, row] * scale
        step_ref[...] = step
        weight_ref[...] = master_ref[...] - step_rate * step
    for k in range(2):
        for part in range(parts):
            leaving(k, part).wait()


def finish(ratio, own, other, bulk, query_master, key_master):
    own_rows, width = query_master.shape
    rows = ratio.shape[0]
    mine = jax.ShapeDtypeStruct((own_rows, width), F32)
    copied = jax.ShapeDtypeStruct((rows, own_rows, width), BF)
    vmem, anywhere = pl.BlockSpec(memory_space=pltpu.VMEM), pl.BlockSpec(memory_space=pl.ANY)
    return pl.pallas_call(
        finish_kernel,
        out_shape=(mine, mine, copied) * 2,
        in_specs=[vmem, vmem, anywhere, anywhere, vmem, vmem],
        out_specs=(vmem, vmem, anywhere) * 2,
        scratch_shapes=[
            pltpu.VMEM(other.shape, BF),
            pltpu.VMEM((rows, 2, own_rows, width), BF),
            pltpu.VMEM((2, rows, own_rows, width), F32),
            pltpu.VMEM((2, rows, own_rows, width), BF),
            pltpu.VMEM((2, 8, width), F32),
            pltpu.SemaphoreType.DMA((2,)),
            pltpu.SemaphoreType.DMA((2, rows // GROUP)),
        ],
        compiler_params=VMEM,
        name="finish",
    )(ratio, own, other, bulk, query_master, key_master)


def body(
    saved_input,
    query_cot,
    key_cot,
    query_master,
    key_master,
    query_basis,
    key_basis,
    query_first,
    query_second,
    key_first,
    key_second,
):
    rows = lax.axis_size(FS)
    depth = lax.axis_size("z")
    tokens, width = query_cot.shape
    low_count = query_first.shape[0]
    ranks = query_basis.shape[1]
    share = tokens // depth
    core = lax.axis_index("c")
    first_core = core == 0

    pieces = lax.all_to_all(saved_input.reshape(depth, share, width), "z", 0, 0, tiled=True)
    own_rows = jnp.concatenate([query_basis, key_basis], axis=1).reshape(2, width, 2 * ranks)
    own_rows = jnp.where(first_core, own_rows[0], own_rows[1])
    basis = lax.all_gather(own_rows, "x", axis=0, tiled=False)
    own_basis = jnp.where(first_core, query_basis, key_basis)
    bulk = jnp.stack(
        [own_basis[:, :width], own_basis[:, width:], query_master.astype(BF), key_master.astype(BF)]
    )
    bulk = lax.all_gather(bulk.reshape(-1, width), FS, axis=0, tiled=True).reshape(rows, 4, -1, width)
    groups = lax.axis_size("y")
    pieces = pieces.reshape(groups, depth // groups, share, width)
    pieces = lax.all_to_all(pieces, "y", 0, 0, tiled=True)
    low = product(pieces, basis).reshape(2 * groups, share, ranks)
    low = lax.all_to_all(low, ("y", "c"), 0, 0, tiled=True)
    low = totals(low, depth)
    low = lax.all_to_all(low, "z", 0, 0, tiled=True).reshape(tokens, ranks)
    own_cot = jnp.where(first_core, query_cot, key_cot)
    other_cot = swapped(jnp.where(first_core, key_cot, query_cot), "c")

    partial = partials(low, own_cot, other_cot, rows, low_count)
    partial = partial.reshape(2 * rows, low_count, width)
    partial = lax.all_to_all(partial, (*FS, "c"), 0, 0, tiled=True)
    *news, ratio = moments(partial, query_first, query_second, key_first, key_second)
    ratio = lax.all_to_all(ratio, FS, 0, 0, tiled=True)

    own_basis = bulk[:, :2]
    other_basis = swapped(own_basis, "c")
    query_step, query_weight, query_copy, key_step, key_weight, key_copy = finish(
        ratio, own_basis, other_basis, bulk, query_master, key_master
    )
    return (
        query_step,
        query_weight,
        query_copy.reshape(D, width),
        news[0],
        news[1],
        key_step,
        key_weight,
        key_copy.reshape(D, width),
        news[2],
        news[3],
    )


def solution(mesh):
    torus = Mesh(mesh.devices.reshape(4, 4, 16, 2), ("y", "x", "z", "c"))
    tp = ("z", "c")
    split = P(FS, tp)
    rows = P(FS, None)
    copied = P(None, tp)
    in_specs = (split,) * 5 + (rows,) * 2 + (split,) * 4
    out_specs = (split, split, copied, split, split) * 2

    return jax.shard_map(body, mesh=torus, in_specs=in_specs, out_specs=out_specs, check_vma=False)
```

```python
import jax
import jax.numpy as jnp
from jax import lax
from jax.experimental import pallas as pl
from jax.experimental.pallas import tpu as pltpu
from jax.sharding import Mesh
from jax.sharding import PartitionSpec as P


D = 4096
HD = 128
FS = ("y", "x")
BF = jnp.bfloat16
F32 = jnp.float32

moment_decay = 0.8
square_decay = 0.9
square_floor = 1.0
norm_floor = 0.01
step_rate = 0.01

VMEM = pltpu.CompilerParams(vmem_limit_bytes=48 * 1024 * 1024)


def sent_to_all(x, axis):
    count = lax.axis_size(axis)
    return lax.all_to_all(jnp.broadcast_to(x[None], (count, *x.shape)), axis, 0, 0, tiled=True)


def swapped(x, axis):
    count = lax.axis_size(axis)
    return lax.ppermute(x, axis, [(i, i ^ 1) for i in range(count)])


def product_kernel(own_ref, other_ref, top_ref, rest_ref, out_ref):
    core = lax.axis_index("c")
    cut = top_ref.shape[1]
    first = core == 0

    def some(z, total):
        own, other = own_ref[z], other_ref[z]
        left = jnp.where(first, own, other)
        right = jnp.where(first, other, own)
        total += jnp.dot(left[:, :cut], top_ref[z], preferred_element_type=F32)
        both = jnp.concatenate([left[:, cut:], right], axis=1)
        return total + jnp.dot(both, rest_ref[z], preferred_element_type=F32)

    total = lax.fori_loop(0, own_ref.shape[0], some, jnp.zeros(out_ref.shape, F32), unroll=4)
    out_ref[...] = total.astype(out_ref.dtype)


def product(own, other, top, rest):
    return pl.pallas_call(
        product_kernel,
        out_shape=jax.ShapeDtypeStruct((own.shape[1], top.shape[-1]), BF),
        in_specs=[pl.BlockSpec(memory_space=pltpu.VMEM)] * 4,
        compiler_params=VMEM,
        name="product",
    )(own, other, top, rest)


def partial_kernel(low_ref, own_ref, other_ref, out_ref):
    core = lax.axis_index("c")
    rows, _, count, width = out_ref.shape
    contract = (((0,), (0,)), ((), ()))
    cots = jnp.concatenate([own_ref[...], other_ref[...]], axis=1)
    both = lax.dot_general(low_ref[...], cots, contract, preferred_element_type=F32).astype(out_ref.dtype)
    out_ref[:, core] = both[:, :width].reshape(rows, count, width)
    out_ref[:, 1 - core] = both[:, width:].reshape(rows, count, width)


def partials(low, own, other, rows, count):
    return pl.pallas_call(
        partial_kernel,
        out_shape=jax.ShapeDtypeStruct((rows, 2, count, own.shape[-1]), BF),
        in_specs=[pl.BlockSpec(memory_space=pltpu.VMEM)] * 3,
        compiler_params=VMEM,
        name="partials",
    )(low, own, other)


def moments_kernel(
    parts_ref,
    query_first_hbm,
    query_second_hbm,
    key_first_hbm,
    key_second_hbm,
    query_first_new_ref,
    query_second_new_ref,
    key_first_new_ref,
    key_second_new_ref,
    ratio_ref,
    olds_ref,
    arrived,
):
    rows = ratio_ref.shape[0]
    outs = ((query_first_new_ref, query_second_new_ref), (key_first_new_ref, key_second_new_ref))
    olds = (query_first_hbm, query_second_hbm, key_first_hbm, key_second_hbm)
    incoming = [pltpu.make_async_copy(old, olds_ref.at[n], arrived.at[n]) for n, old in enumerate(olds)]
    for copy in incoming:
        copy.start()
    sums = []
    for k in range(2):
        projected = parts_ref[k].astype(F32)
        for f in range(1, rows):
            projected += parts_ref[2 * f + k].astype(F32)
        sums.append(projected)
    for copy in incoming:
        copy.wait()
    for k, projected in enumerate(sums):
        first_new = moment_decay * olds_ref[2 * k] + (1.0 - moment_decay) * projected
        second_new = square_decay * olds_ref[2 * k + 1] + (1.0 - square_decay) * projected * projected
        outs[k][0][...] = first_new
        outs[k][1][...] = second_new
        ratio = (first_new / jnp.sqrt(second_new + square_floor)).astype(BF)
        for f in range(rows):
            ratio_ref[f, k] = ratio


def moments(parts, query_first, query_second, key_first, key_second):
    count, width = query_first.shape
    own = jax.ShapeDtypeStruct((count, width), F32)
    ratios = jax.ShapeDtypeStruct((parts.shape[0] // 2, 2, count, width), BF)
    return pl.pallas_call(
        moments_kernel,
        out_shape=(own, own, own, own, ratios),
        in_specs=[pl.BlockSpec(memory_space=pltpu.VMEM)] + [pl.BlockSpec(memory_space=pltpu.HBM)] * 4,
        scratch_shapes=[pltpu.VMEM((4, count, width), F32), pltpu.SemaphoreType.DMA((4,))],
        compiler_params=VMEM,
        name="moments",
    )(parts, query_first, query_second, key_first, key_second)


GROUP = 4


def finish_kernel(
    ratio_ref,
    own_top_ref,
    own_rest_ref,
    other_top_hbm,
    other_rest_hbm,
    masters_hbm,
    query_master_ref,
    key_master_ref,
    query_step_hbm,
    query_weight_hbm,
    query_copy_hbm,
    key_step_hbm,
    key_weight_hbm,
    key_copy_hbm,
    other_top_ref,
    other_rest_ref,
    masters_ref,
    update_top_ref,
    update_rest_ref,
    copies_ref,
    steps_ref,
    weights_ref,
    scales_ref,
    arrived,
    left,
    owned,
):
    core, row = lax.axis_index("c"), lax.axis_index(FS)
    rows, _, count, width = ratio_ref.shape
    ranks = rows * count
    top, rest = own_top_ref.shape[1], own_rest_ref.shape[1]
    tops, rests = pl.ds(0, top), pl.ds(top, rest)
    incoming = [
        pltpu.make_async_copy(other_top_hbm, other_top_ref, arrived.at[0]),
        pltpu.make_async_copy(other_rest_hbm, other_rest_ref, arrived.at[1]),
        pltpu.make_async_copy(masters_hbm, masters_ref, arrived.at[2]),
    ]
    copy_hbms = (query_copy_hbm, key_copy_hbm)

    def leaving(k, part):
        span = pl.ds(part * GROUP, GROUP)
        return pltpu.make_async_copy(copies_ref.at[k, span], copy_hbms[k].at[span], left.at[k, part])

    for copy in incoming:
        copy.start()

    def products(top_ref, rest_ref, k, ratio, part, total):
        span = pl.ds(part * GROUP, GROUP)
        for basis_ref, update_ref, size in ((top_ref, update_top_ref, top), (rest_ref, update_rest_ref, rest)):
            basis = basis_ref[span].reshape(GROUP * size, ranks)
            update = jnp.dot(basis, ratio, preferred_element_type=F32)
            update_ref[k, span] = update.reshape(GROUP, size, width)
            total += jnp.sum((update * update).reshape(GROUP * size // 8, 8, width), axis=0)
        return total

    def scaled(k, total):
        scale = 1.0 / jnp.sqrt(jnp.sum(total, keepdims=True) / (D * HD) + norm_floor)
        scales_ref[k] = jnp.broadcast_to(scale, (8, width))

    def copied(k, part):
        scale = scales_ref[k][:1]
        for n in range(GROUP):
            f = part * GROUP + n
            for span, update_ref in ((tops, update_top_ref), (rests, update_rest_ref)):
                step = update_ref[k, f] * scale
                copies_ref[k, f, span, :] = (masters_ref[f, k, span, :].astype(F32) - step_rate * step).astype(BF)

    def owning(k):
        return (
            pltpu.make_async_copy(steps_ref.at[k], (query_step_hbm, key_step_hbm)[k], owned.at[k, 0]),
            pltpu.make_async_copy(weights_ref.at[k], (query_weight_hbm, key_weight_hbm)[k], owned.at[k, 1]),
        )

    def own(k):
        for n, master_ref in enumerate((query_master_ref, key_master_ref)):

            @pl.when(k == n)
            def _():
                scale = scales_ref[n][:1]
                for span, update_ref in ((tops, update_top_ref), (rests, update_rest_ref)):
                    step = update_ref[n, row] * scale
                    steps_ref[n, span, :] = step
                    weights_ref[n, span, :] = master_ref[span, :] - step_rate * step
                for copy in owning(n):
                    copy.start()

    def sent(k, part):
        for n in range(2):
            pl.when(k == n)(leaving(n, part).start)

    parts = rows // GROUP
    mine, theirs = core, 1 - core
    ratio = ratio_ref[:, mine].reshape(ranks, width)
    total = jnp.zeros((8, width), F32)
    for part in range(parts):
        total = products(own_top_ref, own_rest_ref, mine, ratio, part, total)
    scaled(mine, total)
    own(mine)
    for copy in incoming:
        copy.wait()
    ratio = ratio_ref[:, theirs].reshape(ranks, width)
    total = jnp.zeros((8, width), F32)
    for part in range(parts):
        total = products(other_top_ref, other_rest_ref, theirs, ratio, part, total)
        copied(mine, part)
        sent(mine, part)
    scaled(theirs, total)
    own(theirs)
    for part in range(parts):
        copied(theirs, part)
        sent(theirs, part)
    for k in range(2):
        for copy in owning(k):
            copy.wait()
    for k in range(2):
        for part in range(parts):
            leaving(k, part).wait()


def finish(ratio, own_top, own_rest, other_top, other_rest, masters, query_master, key_master):
    own_rows, width = query_master.shape
    rows = ratio.shape[0]
    top, rest = own_top.shape[1], own_rest.shape[1]
    mine = jax.ShapeDtypeStruct((own_rows, width), F32)
    copied = jax.ShapeDtypeStruct((rows, own_rows, width), BF)
    vmem, anywhere = pl.BlockSpec(memory_space=pltpu.VMEM), pl.BlockSpec(memory_space=pl.ANY)
    return pl.pallas_call(
        finish_kernel,
        out_shape=(mine, mine, copied) * 2,
        in_specs=[vmem, vmem, vmem, anywhere, anywhere, anywhere, vmem, vmem],
        out_specs=(anywhere, anywhere, anywhere) * 2,
        scratch_shapes=[
            pltpu.VMEM(other_top.shape, BF),
            pltpu.VMEM(other_rest.shape, BF),
            pltpu.VMEM(masters.shape, BF),
            pltpu.VMEM((2, rows, top, width), F32),
            pltpu.VMEM((2, rows, rest, width), F32),
            pltpu.VMEM((2, rows, own_rows, width), BF),
            pltpu.VMEM((2, own_rows, width), F32),
            pltpu.VMEM((2, own_rows, width), F32),
            pltpu.VMEM((2, 8, width), F32),
            pltpu.SemaphoreType.DMA((3,)),
            pltpu.SemaphoreType.DMA((2, rows // GROUP)),
            pltpu.SemaphoreType.DMA((2, 2)),
        ],
        compiler_params=VMEM,
        name="finish",
    )(ratio, own_top, own_rest, other_top, other_rest, masters, query_master, key_master)


TOP = 112


def body(
    saved_input,
    query_cot,
    key_cot,
    query_master,
    key_master,
    query_basis,
    key_basis,
    query_first,
    query_second,
    key_first,
    key_second,
):
    rows = lax.axis_size(FS)
    depth = lax.axis_size("z")
    tokens, width = query_cot.shape
    low_count = query_first.shape[0]
    ranks = query_basis.shape[1]
    share = tokens // depth
    core = lax.axis_index("c")
    first_core = core == 0

    pieces = lax.all_to_all(saved_input.reshape(depth, share, width), "z", 0, 0, tiled=True)
    own_basis = jnp.where(first_core, query_basis, key_basis)
    top = lax.all_gather(own_basis[:TOP], FS, axis=0, tiled=True).reshape(rows, TOP, ranks)
    rest = sent_to_all(own_basis[TOP:], FS)
    rest = rest.reshape(rows, -1, ranks)
    other_pieces = swapped(pieces, "c")
    own_cot = jnp.where(first_core, query_cot, key_cot)
    other_cot = swapped(jnp.where(first_core, key_cot, query_cot), "c")
    low = product(pieces, other_pieces, top, rest)
    low = lax.all_gather(low, "z", axis=0, tiled=True)
    masters = sent_to_all(jnp.stack([query_master, key_master]).astype(BF), FS)

    partial = partials(low, own_cot, other_cot, rows, low_count)
    partial = partial.reshape(2 * rows, low_count, width)
    partial = lax.all_to_all(partial, (*FS, "c"), 0, 0, tiled=True)
    *news, ratio = moments(partial, query_first, query_second, key_first, key_second)
    ratio = lax.all_to_all(ratio, FS, 0, 0, tiled=True)

    other_top = swapped(top, "c")
    other_rest = swapped(rest, "c")
    query_step, query_weight, query_copy, key_step, key_weight, key_copy = finish(
        ratio,
        top,
        rest,
        other_top,
        other_rest,
        masters.reshape(rows, 2, -1, width),
        query_master,
        key_master,
    )
    return (
        query_step,
        query_weight,
        query_copy.reshape(D, width),
        news[0],
        news[1],
        key_step,
        key_weight,
        key_copy.reshape(D, width),
        news[2],
        news[3],
    )


def solution(mesh):
    torus = Mesh(mesh.devices.reshape(4, 4, 16, 2), ("y", "x", "z", "c"))
    tp = ("z", "c")
    split = P(FS, tp)
    rows = P(FS, None)
    copied = P(None, tp)
    in_specs = (split,) * 5 + (rows,) * 2 + (split,) * 4
    out_specs = (split, split, copied, split, split) * 2

    return jax.shard_map(body, mesh=torus, in_specs=in_specs, out_specs=out_specs, check_vma=False)
```

```python
import jax
import jax.numpy as jnp
from jax import lax
from jax.experimental import pallas as pl
from jax.experimental.pallas import tpu as pltpu
from jax.sharding import Mesh
from jax.sharding import PartitionSpec as P


D = 4096
HD = 128
FS = ("y", "x")
BF = jnp.bfloat16
F32 = jnp.float32

moment_decay = 0.8
square_decay = 0.9
square_floor = 1.0
norm_floor = 0.01
step_rate = 0.01

VMEM = pltpu.CompilerParams(vmem_limit_bytes=48 * 1024 * 1024)


def sent_to_all(x, axis):
    count = lax.axis_size(axis)
    return lax.all_to_all(jnp.broadcast_to(x[None], (count, *x.shape)), axis, 0, 0, tiled=True)


def swapped(x, axis):
    count = lax.axis_size(axis)
    return lax.ppermute(x, axis, [(i, i ^ 1) for i in range(count)])


def product_kernel(own_ref, other_ref, top_ref, rest_ref, out_ref):
    core = lax.axis_index("c")
    cut = top_ref.shape[1]
    first = core == 0

    def some(z, total):
        own, other = own_ref[z], other_ref[z]
        left = jnp.where(first, own, other)
        right = jnp.where(first, other, own)
        total += jnp.dot(left[:, :cut], top_ref[z], preferred_element_type=F32)
        both = jnp.concatenate([left[:, cut:], right], axis=1)
        return total + jnp.dot(both, rest_ref[z], preferred_element_type=F32)

    total = lax.fori_loop(0, own_ref.shape[0], some, jnp.zeros(out_ref.shape, F32), unroll=4)
    out_ref[...] = total.astype(out_ref.dtype)


def product(own, other, top, rest):
    return pl.pallas_call(
        product_kernel,
        out_shape=jax.ShapeDtypeStruct((own.shape[1], top.shape[-1]), BF),
        in_specs=[pl.BlockSpec(memory_space=pltpu.VMEM)] * 4,
        compiler_params=VMEM,
        name="product",
    )(own, other, top, rest)


def partial_kernel(low_ref, own_ref, other_ref, out_ref):
    core = lax.axis_index("c")
    rows, _, count, width = out_ref.shape
    contract = (((0,), (0,)), ((), ()))
    cots = jnp.concatenate([own_ref[...], other_ref[...]], axis=1)
    both = lax.dot_general(low_ref[...], cots, contract, preferred_element_type=F32).astype(out_ref.dtype)
    out_ref[:, core] = both[:, :width].reshape(rows, count, width)
    out_ref[:, 1 - core] = both[:, width:].reshape(rows, count, width)


def partials(low, own, other, rows, count):
    return pl.pallas_call(
        partial_kernel,
        out_shape=jax.ShapeDtypeStruct((rows, 2, count, own.shape[-1]), BF),
        in_specs=[pl.BlockSpec(memory_space=pltpu.VMEM)] * 3,
        compiler_params=VMEM,
        name="partials",
    )(low, own, other)


def moments_kernel(
    parts_ref,
    query_first_hbm,
    query_second_hbm,
    key_first_hbm,
    key_second_hbm,
    query_first_new_ref,
    query_second_new_ref,
    key_first_new_ref,
    key_second_new_ref,
    ratio_ref,
    olds_ref,
    arrived,
):
    rows = ratio_ref.shape[0]
    outs = ((query_first_new_ref, query_second_new_ref), (key_first_new_ref, key_second_new_ref))
    olds = (query_first_hbm, query_second_hbm, key_first_hbm, key_second_hbm)
    incoming = [pltpu.make_async_copy(old, olds_ref.at[n], arrived.at[n]) for n, old in enumerate(olds)]
    for copy in incoming:
        copy.start()
    sums = []
    for k in range(2):
        projected = parts_ref[k].astype(F32)
        for f in range(1, rows):
            projected += parts_ref[2 * f + k].astype(F32)
        sums.append(projected)
    for copy in incoming:
        copy.wait()
    for k, projected in enumerate(sums):
        first_new = moment_decay * olds_ref[2 * k] + (1.0 - moment_decay) * projected
        second_new = square_decay * olds_ref[2 * k + 1] + (1.0 - square_decay) * projected * projected
        outs[k][0][...] = first_new
        outs[k][1][...] = second_new
        ratio = (first_new / jnp.sqrt(second_new + square_floor)).astype(BF)
        for f in range(rows):
            ratio_ref[f, k] = ratio


def moments(parts, query_first, query_second, key_first, key_second):
    count, width = query_first.shape
    own = jax.ShapeDtypeStruct((count, width), F32)
    ratios = jax.ShapeDtypeStruct((parts.shape[0] // 2, 2, count, width), BF)
    return pl.pallas_call(
        moments_kernel,
        out_shape=(own, own, own, own, ratios),
        in_specs=[pl.BlockSpec(memory_space=pltpu.VMEM)] + [pl.BlockSpec(memory_space=pltpu.HBM)] * 4,
        scratch_shapes=[pltpu.VMEM((4, count, width), F32), pltpu.SemaphoreType.DMA((4,))],
        compiler_params=VMEM,
        name="moments",
    )(parts, query_first, query_second, key_first, key_second)


GROUP = 4


def finish_kernel(
    ratio_hbm,
    own_top_ref,
    own_rest_ref,
    other_top_hbm,
    other_rest_ref,
    masters_hbm,
    query_master_ref,
    key_master_ref,
    query_step_hbm,
    query_weight_hbm,
    query_copy_hbm,
    key_step_hbm,
    key_weight_hbm,
    key_copy_hbm,
    ratio_ref,
    other_top_ref,
    masters_ref,
    update_top_ref,
    update_rest_ref,
    copies_ref,
    steps_ref,
    weights_ref,
    scales_ref,
    arrived,
    left,
    owned,
):
    core, row = lax.axis_index("c"), lax.axis_index(FS)
    rows, _, count, width = ratio_ref.shape
    ranks = rows * count
    top, rest = own_top_ref.shape[1], own_rest_ref.shape[1]
    tops, rests = pl.ds(0, top), pl.ds(top, rest)
    parts = rows // GROUP
    spans = [pl.ds(part * GROUP, GROUP) for part in range(parts)]
    incoming = [
        pltpu.make_async_copy(ratio_hbm, ratio_ref, arrived.at[0]),
        pltpu.make_async_copy(other_top_hbm, other_top_ref, arrived.at[1]),
    ]
    incoming += [
        pltpu.make_async_copy(masters_hbm.at[span], masters_ref.at[span], arrived.at[2 + part])
        for part, span in enumerate(spans)
    ]
    copy_hbms = (query_copy_hbm, key_copy_hbm)

    def leaving(k, part):
        span = pl.ds(part * GROUP, GROUP)
        return pltpu.make_async_copy(copies_ref.at[k, span], copy_hbms[k].at[span], left.at[k, part])

    for copy in incoming:
        copy.start()

    def products(top_ref, rest_ref, k, ratio, part, total):
        span = pl.ds(part * GROUP, GROUP)
        for basis_ref, update_ref, size in ((top_ref, update_top_ref, top), (rest_ref, update_rest_ref, rest)):
            basis = basis_ref[span].reshape(GROUP * size, ranks)
            update = jnp.dot(basis, ratio, preferred_element_type=F32)
            update_ref[k, span] = update.reshape(GROUP, size, width)
            total += jnp.sum((update * update).reshape(GROUP * size // 8, 8, width), axis=0)
        return total

    def scaled(k, total):
        scale = 1.0 / jnp.sqrt(jnp.sum(total, keepdims=True) / (D * HD) + norm_floor)
        scales_ref[k] = jnp.broadcast_to(scale, (8, width))

    def copied(k, part):
        scale = scales_ref[k][:1]
        for n in range(GROUP):
            f = part * GROUP + n
            for span, update_ref in ((tops, update_top_ref), (rests, update_rest_ref)):
                step = update_ref[k, f] * scale
                copies_ref[k, f, span, :] = (masters_ref[f, k, span, :].astype(F32) - step_rate * step).astype(BF)

    def owning(k):
        return (
            pltpu.make_async_copy(steps_ref.at[k], (query_step_hbm, key_step_hbm)[k], owned.at[k, 0]),
            pltpu.make_async_copy(weights_ref.at[k], (query_weight_hbm, key_weight_hbm)[k], owned.at[k, 1]),
        )

    def own(k):
        for n, master_ref in enumerate((query_master_ref, key_master_ref)):

            @pl.when(k == n)
            def _():
                scale = scales_ref[n][:1]
                for span, update_ref in ((tops, update_top_ref), (rests, update_rest_ref)):
                    step = update_ref[n, row] * scale
                    steps_ref[n, span, :] = step
                    weights_ref[n, span, :] = master_ref[span, :] - step_rate * step
                for copy in owning(n):
                    copy.start()

    def sent(k, part):
        for n in range(2):
            pl.when(k == n)(leaving(n, part).start)

    mine, theirs = core, 1 - core
    incoming[0].wait()
    ratio = ratio_ref[:, mine].reshape(ranks, width)
    total = jnp.zeros((8, width), F32)
    for part in range(parts):
        total = products(own_top_ref, own_rest_ref, mine, ratio, part, total)
    scaled(mine, total)
    own(mine)
    incoming[1].wait()
    ratio = ratio_ref[:, theirs].reshape(ranks, width)
    total = jnp.zeros((8, width), F32)
    for part in range(parts):
        total = products(other_top_ref, other_rest_ref, theirs, ratio, part, total)
        incoming[2 + part].wait()
        copied(mine, part)
        sent(mine, part)
    scaled(theirs, total)
    own(theirs)
    for part in range(parts):
        copied(theirs, part)
        sent(theirs, part)
    for k in range(2):
        for copy in owning(k):
            copy.wait()
    for k in range(2):
        for part in range(parts):
            leaving(k, part).wait()


def finish(ratio, own_top, own_rest, other_top, other_rest, masters, query_master, key_master):
    own_rows, width = query_master.shape
    rows = ratio.shape[0]
    top, rest = own_top.shape[1], own_rest.shape[1]
    mine = jax.ShapeDtypeStruct((own_rows, width), F32)
    copied = jax.ShapeDtypeStruct((rows, own_rows, width), BF)
    vmem, anywhere = pl.BlockSpec(memory_space=pltpu.VMEM), pl.BlockSpec(memory_space=pl.ANY)
    return pl.pallas_call(
        finish_kernel,
        out_shape=(mine, mine, copied) * 2,
        in_specs=[anywhere, vmem, vmem, anywhere, vmem, anywhere, vmem, vmem],
        out_specs=(anywhere, anywhere, anywhere) * 2,
        scratch_shapes=[
            pltpu.VMEM(ratio.shape, BF),
            pltpu.VMEM(other_top.shape, BF),
            pltpu.VMEM(masters.shape, BF),
            pltpu.VMEM((2, rows, top, width), F32),
            pltpu.VMEM((2, rows, rest, width), F32),
            pltpu.VMEM((2, rows, own_rows, width), BF),
            pltpu.VMEM((2, own_rows, width), F32),
            pltpu.VMEM((2, own_rows, width), F32),
            pltpu.VMEM((2, 8, width), F32),
            pltpu.SemaphoreType.DMA((2 + rows // GROUP,)),
            pltpu.SemaphoreType.DMA((2, rows // GROUP)),
            pltpu.SemaphoreType.DMA((2, 2)),
        ],
        compiler_params=VMEM,
        name="finish",
    )(ratio, own_top, own_rest, other_top, other_rest, masters, query_master, key_master)


TOP = 120


def body(
    saved_input,
    query_cot,
    key_cot,
    query_master,
    key_master,
    query_basis,
    key_basis,
    query_first,
    query_second,
    key_first,
    key_second,
):
    rows = lax.axis_size(FS)
    depth = lax.axis_size("z")
    tokens, width = query_cot.shape
    low_count = query_first.shape[0]
    ranks = query_basis.shape[1]
    share = tokens // depth
    core = lax.axis_index("c")
    first_core = core == 0

    pieces = lax.all_to_all(saved_input.reshape(depth, share, width), "z", 0, 0, tiled=True)
    own_basis = jnp.where(first_core, query_basis, key_basis)
    top = lax.all_gather(own_basis[:TOP], FS, axis=0, tiled=True).reshape(rows, TOP, ranks)
    rest = sent_to_all(own_basis[TOP:], FS)
    rest = rest.reshape(rows, -1, ranks)
    other_pieces = swapped(pieces, "c")
    own_cot = jnp.where(first_core, query_cot, key_cot)
    other_cot = swapped(jnp.where(first_core, key_cot, query_cot), "c")
    low = product(pieces, other_pieces, top, rest)
    low = lax.all_gather(low, "z", axis=0, tiled=True)
    masters = sent_to_all(jnp.stack([query_master, key_master]).astype(BF), FS)

    partial = partials(low, own_cot, other_cot, rows, low_count)
    partial = partial.reshape(2 * rows, low_count, width)
    partial = lax.all_to_all(partial, (*FS, "c"), 0, 0, tiled=True)
    *news, ratio = moments(partial, query_first, query_second, key_first, key_second)
    ratio = lax.all_to_all(ratio, FS, 0, 0, tiled=True)

    other_top = swapped(top, "c")
    other_rest = swapped(rest, "c")
    query_step, query_weight, query_copy, key_step, key_weight, key_copy = finish(
        ratio,
        top,
        rest,
        other_top,
        other_rest,
        masters.reshape(rows, 2, -1, width),
        query_master,
        key_master,
    )
    return (
        query_step,
        query_weight,
        query_copy.reshape(D, width),
        news[0],
        news[1],
        key_step,
        key_weight,
        key_copy.reshape(D, width),
        news[2],
        news[3],
    )


def solution(mesh):
    torus = Mesh(mesh.devices.reshape(4, 4, 16, 2), ("y", "x", "z", "c"))
    tp = ("z", "c")
    split = P(FS, tp)
    rows = P(FS, None)
    copied = P(None, tp)
    in_specs = (split,) * 5 + (rows,) * 2 + (split,) * 4
    out_specs = (split, split, copied, split, split) * 2

    return jax.shard_map(body, mesh=torus, in_specs=in_specs, out_specs=out_specs, check_vma=False)
```
